256 devices in a mesh: ep: 32 (over z, x), tp: 8 (over y, core).
Axes of the slice: x: 4, y: 4, z: 8, core: 2. Of those that a mesh axis runs over, the one named last changes fastest.
Arguments:
- tokens: bfloat16 [1024, 4096], P('ep'), may hold values from -6 to 6
- mix_gain: bfloat16 [4096], replicated, may hold values from 0.099609375 to 1.8984375
- query_weight: bfloat16 [4096, 1024], P(None, 'tp'), may hold values from -0.09375 to 0.09375
- key_weight: bfloat16 [4096, 1024], P(None, 'tp'), may hold values from -0.09375 to 0.09375
- value_weight: bfloat16 [4096, 1024], P(None, 'tp'), may hold values from -0.09375 to 0.09375
- decay_weight: bfloat16 [4096, 8], replicated, may hold values from -0.09375 to 0.09375
- strength_weight: bfloat16 [4096, 8], replicated, may hold values from -0.09375 to 0.09375
- decay_rate: float32 [8], P('tp'), may hold values from 0.03 to 3
- head_gain: bfloat16 [128], replicated, may hold values from 0.099609375 to 1.8984375
- memory_state: float32 [1024, 8, 128, 128], P('ep', 'tp'), may hold values from -0.6 to 0.6
- output_weight: bfloat16 [1024, 4096], P('tp'), may hold values from -0.1875 to 0.1875
- ffn_gain: bfloat16 [4096], replicated, may hold values from 0.099609375 to 1.8984375
- routing: int32 [1024, 2], P('ep'), may hold values from 0 to 31, all different within a row; in each aligned block of 32 rows (0 to 31, 32 to 63, ...) at most 4 rows name the same one
- route_weight: float32 [1024, 2], P('ep'), may hold values from 0.1 to 1
- expert_gate: bfloat16 [32, 4096, 2048], P('ep', None, 'tp'), may hold values from -0.25 to 0.25
- expert_up: bfloat16 [32, 4096, 2048], P('ep', None, 'tp'), may hold values from -0.25 to 0.25
- expert_down: bfloat16 [32, 2048, 4096], P('ep', 'tp'), may hold values from -0.03125 to 0.03125
Outputs:
- layer_out: bfloat16 [1024, 4096], P('ep', 'tp')
- new_state: float32 [1024, 8, 128, 128], P('ep', 'tp')
The draws below stay inside these ranges and needn't reach their ends.
Inputs may be any that keep to these rules, and one draw needn't show every extreme that they name: `routing`: each row names 2 different experts. In each aligned block of 32 rows (the rows of one device) no expert is named more than 4 times, a bound that some block reaches.
All inputs are finite; a program needn't handle non-finite values.
Results may differ from the reference program's by a relative error of at most 0.019.
Values may be sent and summed in bfloat16 or wider, within the bound.
No kernel may reach another device: no remote copies, remote signals or barrier semaphores. Data moves between devices by JAX's collectives and lax.ppermute only.
A program may use at most 64 MiB of HBM per device.

```python
import math
import jax
import jax.numpy as jnp
import numpy as np
from jax import lax

D = 4096
HEADS = 8
HEAD = 128
FF = 2048
TOP_K = 2
B_DEV = 32
EXPERTS = 32
CAP = 4
TOKENS = 1024
N_EP = 32
N_TP = 8


def shard_levels(stream_key, extent, pieces, smallest, high):
    factor_of = 1.0
    for dim, shards_of in pieces:
        heights = jax.random.uniform(jax.random.fold_in(jax.random.fold_in(stream_key, 6), dim), (shards_of,), jnp.float32, smallest / len(pieces), high / len(pieces))
        factor_of = factor_of * jnp.repeat(jnp.exp(heights), extent[dim] // shards_of).reshape((-1,) + (1,) * (len(extent) - 1 - dim))
    return factor_of


def shared_out(own_key, own, number, rows, count, top, limit, slope):
    sequence = jax.random.permutation(own_key, count)
    crowded, common = portions_of(count, rows * top, limit, slope, True), portions_of(count, rows * top, limit, slope, False)
    places = jnp.arange(count)

    def named(lengths, turn):
        used = int((lengths > 0).sum())
        fixed = max(1, used // 4)
        shifted = fixed + (places - fixed + turn * (used - fixed)) % max(1, count - fixed)
        return jnp.zeros((count,), jnp.int32).at[sequence[jnp.where(places < fixed, places, shifted)]].set(jnp.asarray(lengths, jnp.int32))

    lengths = jnp.where(number % 4 == 0, named(crowded, number // 4), named(common, number - number // 4 - 1))
    mixed = jax.random.permutation(jax.random.fold_in(own, 3), count)
    donor, taker = mixed[0:count // 2 * 2:2], mixed[1:count // 2 * 2:2]
    room = jnp.minimum(lengths[donor] - 1, limit - lengths[taker]) // 2
    room = jnp.where((donor == sequence[0]) | (taker == sequence[0]) | (lengths[taker] == 0), 0, jnp.maximum(room, 0))
    shifted = jax.random.randint(jax.random.fold_in(own, 4), (count // 2,), 0, 1 << 20) % (room + 1)
    lengths = lengths.at[donor].add(-shifted).at[taker].add(shifted)
    labels = jnp.searchsorted(jnp.cumsum(lengths), jnp.arange(rows * top), side="right").astype(jnp.int32)
    listing = labels.reshape(top, rows).T
    listing = listing[jax.random.permutation(jax.random.fold_in(own, 1), rows)]
    turn = jax.random.randint(jax.random.fold_in(own, 2), (rows, 1), 0, top)
    return jnp.take_along_axis(listing, (jnp.arange(top)[None, :] + turn) % top, axis=1)


def portions_of(amount, total, bound, slope, full):
    weights = [(1 << 20) // math.isqrt(standing ** slope) + 1 for standing in range(1, amount + 1)]
    largest = bound if full else min(bound, max(-(-total // amount), total * weights[0] // sum(weights)))
    least = 1 if total - largest >= amount - 1 else 0
    counts, rest = [largest] + [least] * (amount - 1), total - largest - least * (amount - 1)
    while rest > 0:
        candidates = [i for i in range(1, amount) if counts[i] < largest] or [i for i in range(1, amount) if counts[i] < bound]
        mass, remaining = sum([weights[i] for i in candidates]), rest
        for i in candidates:
            addition = min(bound - counts[i], max(1, remaining * weights[i] // mass), rest)
            counts[i] = counts[i] + addition
            rest = rest - addition
    return np.array(counts)


def scatter_about(key, extent, scale, bound, split=(), kind=jnp.bfloat16):
    array = scale * jax.random.normal(key, extent, jnp.float32)
    if split:
        array = array * shard_levels(key, extent, split, -0.22, 0.18)
    return jnp.clip(array, -bound, bound).astype(kind)


def setup_inputs(seed: int = 0) -> dict:
    streams_of = jax.random.split(jax.random.key(seed), 18)
    tokens = scatter_about(streams_of[0], (TOKENS, D), 1.0, 6.0, ((0, 32),))
    mix_gain = jnp.clip(1.0 + 0.18 * jax.random.normal(streams_of[1], (D,), jnp.float32), 0.099609375, 1.8984375).astype(jnp.bfloat16)
    query_weight = scatter_about(streams_of[2], (D, HEADS * HEAD), D ** -0.5, 0.09375, ((1, 8),))
    key_weight = scatter_about(streams_of[3], (D, HEADS * HEAD), D ** -0.5, 0.09375, ((1, 8),))
    value_weight = scatter_about(streams_of[4], (D, HEADS * HEAD), D ** -0.5, 0.09375, ((1, 8),))
    decay_weight = scatter_about(streams_of[5], (D, HEADS), D ** -0.5, 0.09375)
    strength_weight = scatter_about(streams_of[6], (D, HEADS), D ** -0.5, 0.09375)
    decay_rate = jnp.clip(jnp.exp(math.log(3.0) - 4.6051702 * jax.random.uniform(streams_of[7], (HEADS,), jnp.float32) ** shard_levels(streams_of[7], (HEADS,), ((0, 8),), -0.2, 0.2)), 0.03, 3.0)
    head_gain = jnp.clip(1.0 + 0.18 * jax.random.normal(streams_of[8], (HEAD,), jnp.float32), 0.099609375, 1.8984375).astype(jnp.bfloat16)
    memory_state = scatter_about(streams_of[9], (TOKENS, HEADS, HEAD, HEAD), 0.1, 0.6, ((0, 32), (1, 8)), jnp.float32)
    output_weight = scatter_about(streams_of[10], (HEADS * HEAD, D), (HEADS * HEAD) ** -0.5, 0.1875, ((0, 8),))
    ffn_gain = jnp.clip(1.0 + 0.18 * jax.random.normal(streams_of[11], (D,), jnp.float32), 0.099609375, 1.8984375).astype(jnp.bfloat16)
    routing_keys = jax.random.split(jax.random.fold_in(streams_of[12], 1), TOKENS // B_DEV)
    routing_turns = jax.random.permutation(jax.random.fold_in(streams_of[12], 3), TOKENS // B_DEV)
    routing = jax.vmap(lambda own, number: shared_out(jax.random.fold_in(streams_of[12], 2), own, number, B_DEV, EXPERTS, TOP_K, CAP, 2))(routing_keys, routing_turns).reshape((TOKENS, TOP_K))
    route_weight = jnp.clip(jnp.exp(math.log(1.0) - 2.3025851 * jax.random.uniform(streams_of[13], (TOKENS, TOP_K), jnp.float32) ** shard_levels(streams_of[13], (TOKENS, TOP_K), ((0, 32),), -0.2, 0.2)), 0.1, 1.0)
    expert_gate = scatter_about(streams_of[14], (EXPERTS, D, FF), (D // 9) ** -0.5, 0.25, ((0, 32), (2, 8)))
    expert_up = scatter_about(streams_of[15], (EXPERTS, D, FF), (D // 9) ** -0.5, 0.25, ((0, 32), (2, 8)))
    expert_down = scatter_about(streams_of[16], (EXPERTS, FF, D), (FF * 16) ** -0.5, 0.03125, ((0, 32), (1, 8)))
    return dict(tokens=tokens, mix_gain=mix_gain, query_weight=query_weight, key_weight=key_weight, value_weight=value_weight, decay_weight=decay_weight, strength_weight=strength_weight, decay_rate=decay_rate, head_gain=head_gain, memory_state=memory_state, output_weight=output_weight, ffn_gain=ffn_gain, routing=routing, route_weight=route_weight, expert_gate=expert_gate, expert_up=expert_up, expert_down=expert_down)


epsilon = 1e-06
clamp_limit = 7.0
swish_alpha = 1.702

def rms_scale(rows, gain):
    values = rows.astype(jnp.float32)
    scaled = values * lax.rsqrt(lax.optimization_barrier(jnp.mean(values * values, axis=-1, keepdims=True)) + epsilon)
    return (scaled * gain.astype(jnp.float32)).astype(jnp.bfloat16)

def round_keep(rounded):
    return lax.optimization_barrier(rounded).astype(jnp.float32)

def unit_rows(values):
    return values * lax.rsqrt(lax.optimization_barrier(jnp.sum(values * values, axis=-1, keepdims=True)) + epsilon)

def delta_step(projected, decay_log, strength, memory_state, head_gain):
    queries = unit_rows(jax.nn.silu(projected[:, 0])) * projected.shape[-1] ** (-0.5)
    keys_unit = unit_rows(jax.nn.silu(projected[:, 1]))
    values_new = jax.nn.silu(projected[:, 2])
    retained = memory_state * jnp.exp(decay_log)[:, :, None, None]
    recalled = jnp.einsum('thd,thde->the', keys_unit, retained, precision=lax.Precision.HIGHEST)
    corrected = strength[:, :, None] * (values_new - recalled)
    updated = retained + keys_unit[:, :, :, None] * corrected[:, :, None, :]
    readout = jnp.einsum('thd,thde->the', queries, updated, precision=lax.Precision.HIGHEST)
    scaled = readout * lax.rsqrt(lax.optimization_barrier(jnp.mean(readout * readout, axis=-1, keepdims=True)) + epsilon)
    mixed = scaled * head_gain.astype(jnp.float32)
    return (mixed.astype(jnp.bfloat16), updated)

def clamped_unit(gate_pre, up_pre):
    gate_cut = jnp.minimum(gate_pre, clamp_limit)
    up_cut = jnp.clip(up_pre, -clamp_limit, clamp_limit)
    return ((up_cut + 1.0) * gate_cut * jax.nn.sigmoid(swish_alpha * gate_cut)).astype(jnp.bfloat16)

def reference(tokens, mix_gain, query_weight, key_weight, value_weight, decay_weight, strength_weight, decay_rate, head_gain, memory_state, output_weight, ffn_gain, routing, route_weight, expert_gate, expert_up, expert_down):
    normed = rms_scale(tokens, mix_gain)
    joined = jnp.concatenate([query_weight, key_weight, value_weight], axis=1)
    projected = round_keep(jnp.dot(normed, joined, preferred_element_type=jnp.float32).astype(jnp.bfloat16))
    projected = projected.reshape(TOKENS, 3, HEADS, HEAD)
    decay_pre = jnp.dot(normed, decay_weight, preferred_element_type=jnp.float32)
    decay_log = -decay_rate[None, :] * jax.nn.softplus(decay_pre)
    strength = jax.nn.sigmoid(jnp.dot(normed, strength_weight, preferred_element_type=jnp.float32))
    mixed, new_state = delta_step(projected, decay_log, strength, memory_state, head_gain)
    mixed = mixed.reshape(TOKENS, HEADS * HEAD)
    shard_width = HEADS * HEAD // N_TP

    def add_shard(shard_id, running):
        offset = (shard_id * shard_width).astype(jnp.int32)
        rows_part = lax.dynamic_slice_in_dim(mixed, offset, shard_width, 1)
        weight_part = lax.dynamic_slice_in_dim(output_weight, offset, shard_width, 0)
        partial_term = jnp.dot(rows_part, weight_part, preferred_element_type=jnp.float32)
        return running + round_keep(partial_term.astype(jnp.bfloat16))
    mix_sum = lax.fori_loop(0, N_TP, add_shard, jnp.zeros((TOKENS, D), jnp.float32))
    residual = (tokens.astype(jnp.float32) + mix_sum).astype(jnp.bfloat16)
    ffn_in = rms_scale(residual, ffn_gain)
    pairs = B_DEV * TOP_K
    chosen = routing.reshape(N_EP, pairs)
    marks = (chosen[:, :, None] == jnp.arange(EXPERTS, dtype=jnp.int32)[None, None, :]).astype(jnp.int32)
    order_rank = lax.optimization_barrier(jnp.sum((jnp.cumsum(marks, axis=1) - 1) * marks, axis=2))
    block_id = jnp.arange(N_EP, dtype=jnp.int32)[:, None]
    position = (chosen * (N_EP * CAP) + block_id * CAP + order_rank).reshape(-1).astype(jnp.int32)
    owner = (block_id * B_DEV + jnp.arange(pairs, dtype=jnp.int32)[None, :] // TOP_K).reshape(-1).astype(jnp.int32)
    buffer = jnp.zeros((EXPERTS * N_EP * CAP, D), jnp.bfloat16).at[position].set(ffn_in[owner])
    buffer = buffer.reshape(EXPERTS, N_EP * CAP, D)
    ff_width = FF // N_TP

    def run_expert(expert_id):
        expert_rows = buffer[expert_id]
        gate_pre = jnp.dot(expert_rows, expert_gate[expert_id], preferred_element_type=jnp.float32)
        up_pre = jnp.dot(expert_rows, expert_up[expert_id], preferred_element_type=jnp.float32)
        hidden = clamped_unit(gate_pre, up_pre)
        down_rows = expert_down[expert_id]
        running = jnp.zeros((N_EP * CAP, D), jnp.float32)
        for shard_id in range(N_TP):
            partial_term = jnp.dot(hidden[:, shard_id * ff_width:(shard_id + 1) * ff_width], down_rows[shard_id * ff_width:(shard_id + 1) * ff_width], preferred_element_type=jnp.float32)
            running = running + round_keep(partial_term.astype(jnp.bfloat16))
        return running.astype(jnp.bfloat16)
    outputs = lax.map(run_expert, jnp.arange(EXPERTS, dtype=jnp.int32)).reshape(EXPERTS * N_EP * CAP, D)
    picked = outputs[position].astype(jnp.float32).reshape(TOKENS, TOP_K, D)
    routed = lax.optimization_barrier(jnp.sum(picked * route_weight[:, :, None], axis=1))
    layer_out = (residual.astype(jnp.float32) + routed).astype(jnp.bfloat16)
    return (layer_out, new_state)
```

```python
import jax
import jax.numpy as jnp
from jax import lax
from jax.experimental import pallas as pl
from jax.experimental.pallas import tpu as pltpu
from jax.sharding import PartitionSpec as P

epsilon = 1e-06
clamp_limit = 7.0
swish_alpha = 1.702
f32 = jnp.float32
bf16 = jnp.bfloat16


VMEM = pltpu.VMEM
SMEM = pltpu.SMEM


def in_vmem():
    return pl.BlockSpec(memory_space=VMEM)


def in_smem():
    return pl.BlockSpec(memory_space=SMEM)


def in_hbm():
    return pl.BlockSpec(memory_space=pltpu.HBM)


def pinned(array):
    return pltpu.with_memory_space_constraint(array, pltpu.HBM)


def shaped(shape, dtype):
    return jax.ShapeDtypeStruct(shape, dtype)


def silu(values):
    return values * jax.nn.sigmoid(values)


def mixer_kernel(
    lane_ref,
    rate_ref,
    tokens_ref,
    gain_ref,
    decay_ref,
    strength_ref,
    head_gain_ref,
    query_hbm,
    key_hbm,
    value_hbm,
    state_hbm,
    out_hbm,
    send_ref,
    keep_ref,
    retain_ref,
    corrected_ref,
    keys_ref,
    proj_s,
    state_s,
    out_s,
    recall_s,
    read_s,
    sems,
):
    rows, width = tokens_ref.shape
    head = head_gain_ref.shape[-1]
    chunks = 4
    step = width // chunks
    copies = []
    for c in range(chunks):
        for n, source in enumerate((query_hbm, key_hbm, value_hbm)):
            copies.append(
                pltpu.make_async_copy(
                    source.at[pl.ds(c * step, step), :],
                    proj_s.at[pl.ds(c * step, step), pl.ds(n * head, head)],
                    sems.at[c * 3 + n],
                )
            )
    state_copy = pltpu.make_async_copy(state_hbm, state_s, sems.at[chunks * 3])
    out_copy = pltpu.make_async_copy(out_hbm, out_s, sems.at[chunks * 3 + 1])
    for copy in copies:
        copy.start()
    state_copy.start()
    out_copy.start()

    values = tokens_ref[...].astype(f32)
    scale = lax.rsqrt(jnp.mean(values * values, axis=-1, keepdims=True) + epsilon)
    normed = (values * scale * gain_ref[...].astype(f32)).astype(bf16)

    def gate_of(weights):
        return lax.dot_general(
            normed, weights, (((1,), (1,)), ((), ())), preferred_element_type=f32
        )

    lane = lane_ref[0]
    heads = decay_ref.shape[0]
    column = lax.broadcasted_iota(jnp.int32, (rows, heads), 1) == lane

    def own(pre):
        return jnp.sum(jnp.where(column, pre, 0.0), axis=1, keepdims=True)

    decay_pre = own(gate_of(decay_ref[...]))
    strength = jax.nn.sigmoid(own(gate_of(strength_ref[...])))
    softplus = jnp.maximum(decay_pre, 0.0) + jnp.log1p(jnp.exp(-jnp.abs(decay_pre)))
    retain = jnp.exp(-rate_ref[0] * softplus)

    total = jnp.zeros((rows, 3 * head), f32)
    for c in range(chunks):
        for copy in copies[3 * c : 3 * c + 3]:
            copy.wait()
        total = total + jnp.dot(
            normed[:, c * step : (c + 1) * step],
            proj_s[pl.ds(c * step, step), :],
            preferred_element_type=f32,
        )
    projected = total.astype(bf16).astype(f32)
    query = silu(projected[:, :head])
    key = silu(projected[:, head : 2 * head])
    value = silu(projected[:, 2 * head :])
    query = query * lax.rsqrt(jnp.sum(query * query, axis=-1, keepdims=True) + epsilon)
    query = query * head ** (-0.5)
    key = key * lax.rsqrt(jnp.sum(key * key, axis=-1, keepdims=True) + epsilon)
    match = jnp.sum(query * key, axis=-1, keepdims=True)

    fill = jnp.zeros((head - rows, head), f32)
    query_t = jnp.transpose(jnp.concatenate([query, fill], axis=0))
    key_t = jnp.transpose(jnp.concatenate([key, fill], axis=0))
    keys_ref[...] = key_t
    state_copy.wait()
    for t in range(rows):
        block = state_s[t]
        recall_s[pl.ds(t, 1), :] = jnp.sum(block * key_t[:, t : t + 1], axis=0, keepdims=True)
        read_s[pl.ds(t, 1), :] = jnp.sum(block * query_t[:, t : t + 1], axis=0, keepdims=True)
    corrected = strength * (value - retain * recall_s[...])
    readout = retain * read_s[...] + match * corrected
    retain_ref[...] = jnp.broadcast_to(retain, (rows, head))
    corrected_ref[...] = corrected
    scaled = readout * lax.rsqrt(jnp.mean(readout * readout, axis=-1, keepdims=True) + epsilon)
    mixed = (scaled * head_gain_ref[...].astype(f32)).astype(bf16)

    out_copy.wait()
    share = send_ref.shape[-1]
    for k in range(4):
        near = (lane ^ (2 * k)) * share
        far = (lane ^ (2 * k + 1)) * share
        send_ref[k] = jnp.dot(
            mixed, out_s[:, pl.ds(pl.multiple_of(far, 128), share)], preferred_element_type=f32
        ).astype(bf16)
        keep_ref[k] = jnp.dot(
            mixed, out_s[:, pl.ds(pl.multiple_of(near, 128), share)], preferred_element_type=f32
        ).astype(bf16)


def state_kernel(retain_ref, corrected_ref, keys_ref, state_hbm, new_hbm, old_s, new_s, sems):
    rows = old_s.shape[0]
    parts = 4
    step = rows // parts

    def window(i):
        return pl.ds(i * step, step)

    loads = [
        pltpu.make_async_copy(state_hbm.at[window(i)], old_s.at[window(i)], sems.at[i])
        for i in range(parts)
    ]
    stores = [
        pltpu.make_async_copy(new_s.at[window(i)], new_hbm.at[window(i)], sems.at[parts + i])
        for i in range(parts)
    ]
    for load in loads:
        load.start()
    for i in range(parts):
        loads[i].wait()
        for t in range(i * step, (i + 1) * step):
            new_s[t] = (
                old_s[t] * retain_ref[pl.ds(t, 1), :]
                + keys_ref[:, t : t + 1] * corrected_ref[pl.ds(t, 1), :]
            )
        stores[i].start()
    for store in stores:
        store.wait()


def pair_sum_kernel(keep_ref, recv_ref, *out_refs):
    for k, out in enumerate(out_refs):
        out[...] = (keep_ref[k].astype(f32) + recv_ref[k].astype(f32)).astype(bf16)


def residual_kernel(
    lane_ref, tokens_ref, place_ref, a_ref, b_ref, c_ref, d_ref, own_ref, out_ref
):
    share = own_ref.shape[-1]
    start = pl.multiple_of(lane_ref[0] * share, 128)
    mix = (a_ref[...].astype(f32) + b_ref[...].astype(f32)) + (
        c_ref[...].astype(f32) + d_ref[...].astype(f32)
    )
    own = (tokens_ref[:, pl.ds(start, share)].astype(f32) + mix).astype(bf16)
    own_ref[...] = own
    out_ref[...] = jnp.dot(place_ref[...], own, preferred_element_type=f32).astype(bf16)


def expert_kernel(
    lane_ref,
    gain_ref,
    *refs,
):
    pieces = refs[:8]
    gate_hbm, up_hbm, down_hbm, send_ref, keep_ref, gate_s, up_s, down_s, sems = refs[8:]
    rows, share = pieces[0].shape
    lane = lane_ref[0]
    starts = [pl.multiple_of((lane ^ k) * share, 128) for k in range(8)]
    gate_copies = []
    up_copies = []
    for k in range(8):
        window = pl.ds(starts[k], share)
        gate_copies.append(
            pltpu.make_async_copy(gate_hbm.at[window, :], gate_s.at[k], sems.at[k])
        )
        up_copies.append(pltpu.make_async_copy(up_hbm.at[window, :], up_s.at[k], sems.at[8 + k]))
        gate_copies[k].start()
        up_copies[k].start()
    down_copy = pltpu.make_async_copy(down_hbm, down_s, sems.at[16])
    down_copy.start()

    square = jnp.zeros((rows, 1), f32)
    for k in range(8):
        values = pieces[k][...].astype(f32)
        square = square + jnp.sum(values * values, axis=-1, keepdims=True)
    scale = lax.rsqrt(square / (8 * share) + epsilon)
    gate_pre = jnp.zeros((rows, gate_s.shape[-1]), f32)
    up_pre = jnp.zeros((rows, gate_s.shape[-1]), f32)
    for k in range(8):
        gain = gain_ref[:, pl.ds(starts[k], share)].astype(f32)
        fed = (pieces[k][...].astype(f32) * scale * gain).astype(bf16)
        gate_copies[k].wait()
        gate_pre = gate_pre + jnp.dot(fed, gate_s[k], preferred_element_type=f32)
        up_copies[k].wait()
        up_pre = up_pre + jnp.dot(fed, up_s[k], preferred_element_type=f32)
    gate_cut = jnp.minimum(gate_pre, clamp_limit)
    up_cut = jnp.clip(up_pre, -clamp_limit, clamp_limit)
    hidden = ((up_cut + 1.0) * gate_cut * jax.nn.sigmoid(swish_alpha * gate_cut)).astype(bf16)
    down_copy.wait()
    for k in range(4):
        send_ref[k] = jnp.dot(
            hidden, down_s[:, pl.ds(starts[2 * k + 1], share)], preferred_element_type=f32
        ).astype(bf16)
        keep_ref[k] = jnp.dot(
            hidden, down_s[:, pl.ds(starts[2 * k], share)], preferred_element_type=f32
        ).astype(bf16)


def total_kernel(a_ref, b_ref, c_ref, d_ref, out_ref):
    out_ref[...] = (
        (a_ref[...].astype(f32) + b_ref[...].astype(f32))
        + (c_ref[...].astype(f32) + d_ref[...].astype(f32))
    ).astype(bf16)


def combine_kernel(own_ref, first_ref, second_ref, weight_ref, back_ref, out_ref):
    back = back_ref[...]
    first = jnp.dot(first_ref[...], back, preferred_element_type=f32)
    second = jnp.dot(second_ref[...], back, preferred_element_type=f32)
    weight = weight_ref[...]
    routed = first * weight[:, 0:1] + second * weight[:, 1:2]
    out_ref[...] = (own_ref[...].astype(f32) + routed).astype(bf16)


def on_device(
    tokens,
    mix_gain,
    query_weight,
    key_weight,
    value_weight,
    decay_weight,
    strength_weight,
    decay_rate,
    head_gain,
    memory_state,
    output_weight,
    ffn_gain,
    routing,
    route_weight,
    expert_gate,
    expert_up,
    expert_down,
):
    groups = lax.axis_size("ep")
    lane = lax.axis_index("tp").astype(jnp.int32).reshape(1)
    rows, width = tokens.shape
    head = memory_state.shape[-1]
    share = width // 8
    hidden_units = expert_gate.shape[-1]
    top = routing.shape[1]
    capacity = 2 * rows * top // groups
    slots = groups * capacity
    limits = pltpu.CompilerParams(vmem_limit_bytes=24 * 2**20)

    def across(array, flip):
        return lax.ppermute(array, "tp", [(i, i ^ flip) for i in range(8)])

    state = memory_state.reshape(rows, head, head)
    send, keep, retain, corrected, keys = pl.pallas_call(
        mixer_kernel,
        out_shape=(
            shaped((4, rows, share), bf16),
            shaped((4, rows, share), bf16),
            shaped((rows, head), f32),
            shaped((rows, head), f32),
            shaped((head, head), f32),
        ),
        in_specs=[in_smem(), in_smem()] + [in_vmem()] * 5 + [in_hbm()] * 5,
        out_specs=(in_vmem(),) * 5,
        scratch_shapes=[
            VMEM((width, 3 * head), bf16),
            VMEM((rows, head, head), f32),
            VMEM((head, width), bf16),
            VMEM((rows, head), f32),
            VMEM((rows, head), f32),
            pltpu.SemaphoreType.DMA((14,)),
        ],
        compiler_params=limits,
        name="mixer",
    )(
        lane,
        decay_rate,
        tokens,
        mix_gain.reshape(1, width),
        decay_weight.T,
        strength_weight.T,
        head_gain.reshape(1, head),
        pinned(query_weight),
        pinned(key_weight),
        pinned(value_weight),
        pinned(state),
        pinned(output_weight),
    )
    recv = across(send, 1)

    def pair_sums(keep, recv):
        shape = keep.shape[1:]
        return pl.pallas_call(
            pair_sum_kernel,
            out_shape=(shaped(shape, bf16),) * 4,
            in_specs=[in_vmem()] * 2,
            out_specs=(in_vmem(),) * 4,
            compiler_params=limits,
            name="pair_sum",
        )(keep, recv)

    sums = pair_sums(keep, recv)
    gathered = [sums[0]] + [across(sums[k], 2 * k) for k in (1, 2, 3)]

    new_state = pl.pallas_call(
        state_kernel,
        out_shape=shaped(state.shape, f32),
        in_specs=[in_vmem()] * 3 + [in_hbm()],
        out_specs=in_hbm(),
        scratch_shapes=[
            VMEM(state.shape, f32),
            VMEM(state.shape, f32),
            pltpu.SemaphoreType.DMA((8,)),
        ],
        compiler_params=limits,
        name="state",
    )(retain, corrected, keys, pinned(state))

    chosen = routing.reshape(-1)
    pairs = chosen.shape[0]
    order = jnp.arange(pairs, dtype=jnp.int32)
    earlier = (chosen[:, None] == chosen[None, :]) & (order[None, :] < order[:, None])
    rank = jnp.sum(earlier.astype(jnp.int32), axis=1)
    slot = (chosen * capacity + rank).reshape(rows, top)
    line = jnp.arange(slots, dtype=jnp.int32)
    picks = (slot[:, :, None] == line[None, None, :]).astype(bf16)
    first, second = picks[:, 0], picks[:, 1]
    place = (first + second).T

    own, outgoing = pl.pallas_call(
        residual_kernel,
        out_shape=(shaped((rows, share), bf16), shaped((slots, share), bf16)),
        in_specs=[in_smem()] + [in_vmem()] * 6,
        out_specs=(in_vmem(),) * 2,
        compiler_params=limits,
        name="residual",
    )(lane, tokens, place, *gathered)

    def exchanged(array):
        blocks = array.reshape(groups, capacity, share)
        return lax.all_to_all(blocks, "ep", 0, 0, tiled=True).reshape(slots, share)

    arrived = exchanged(outgoing)
    near = {0: arrived}
    for k in (2, 1, 3):
        near[2 * k] = across(arrived, 2 * k)
    pieces = []
    for k in range(4):
        pieces.append(near[2 * k])
        pieces.append(across(near[2 * k], 1))

    send, keep = pl.pallas_call(
        expert_kernel,
        out_shape=(shaped((4, slots, share), bf16),) * 2,
        in_specs=[in_smem()] + [in_vmem()] * 9 + [in_hbm()] * 3,
        out_specs=(in_vmem(),) * 2,
        scratch_shapes=[
            VMEM((8, share, hidden_units), bf16),
            VMEM((8, share, hidden_units), bf16),
            VMEM((hidden_units, width), bf16),
            pltpu.SemaphoreType.DMA((17,)),
        ],
        compiler_params=limits,
        name="expert",
    )(
        lane,
        ffn_gain.reshape(1, width),
        *pieces,
        pinned(expert_gate.reshape(width, hidden_units)),
        pinned(expert_up.reshape(width, hidden_units)),
        pinned(expert_down.reshape(hidden_units, width)),
    )
    recv = across(send, 1)
    sums = pair_sums(keep, recv)
    gathered = [sums[0]] + [across(sums[k], 2 * k) for k in (1, 2, 3)]
    expert_out = pl.pallas_call(
        total_kernel,
        out_shape=shaped((slots, share), bf16),
        in_specs=[in_vmem()] * 4,
        out_specs=in_vmem(),
        compiler_params=limits,
        name="total",
    )(*gathered)
    back = exchanged(expert_out)
    layer_out = pl.pallas_call(
        combine_kernel,
        out_shape=shaped((rows, share), bf16),
        in_specs=[in_vmem()] * 5,
        out_specs=in_vmem(),
        compiler_params=limits,
        name="combine",
    )(own, first, second, route_weight, back)
    return layer_out, new_state.reshape(memory_state.shape)


def solution(mesh):
    placed = (
        P("ep", None),
        P(),
        P(None, "tp"),
        P(None, "tp"),
        P(None, "tp"),
        P(),
        P(),
        P("tp"),
        P(),
        P("ep", "tp", None, None),
        P("tp", None),
        P(),
        P("ep", None),
        P("ep", None),
        P("ep", None, "tp"),
        P("ep", None, "tp"),
        P("ep", "tp", None),
    )
    return jax.shard_map(
        on_device,
        mesh=mesh,
        in_specs=placed,
        out_specs=(P("ep", "tp"), P("ep", "tp", None, None)),
        check_vma=False,
    )
```

```python
from functools import partial

import jax
import jax.numpy as jnp
from jax import lax
from jax.experimental import pallas as pl
from jax.experimental.pallas import tpu as pltpu
from jax.sharding import PartitionSpec as P

epsilon = 1e-06
clamp_limit = 7.0
swish_alpha = 1.702
f32 = jnp.float32
bf16 = jnp.bfloat16


VMEM = pltpu.VMEM
SMEM = pltpu.SMEM


def in_vmem():
    return pl.BlockSpec(memory_space=VMEM)


def in_smem():
    return pl.BlockSpec(memory_space=SMEM)


def in_hbm():
    return pl.BlockSpec(memory_space=pltpu.HBM)


def in_any():
    return pl.BlockSpec(memory_space=pl.ANY)


def pinned(array):
    return pltpu.with_memory_space_constraint(array, pltpu.HBM)


def shaped(shape, dtype):
    return jax.ShapeDtypeStruct(shape, dtype)


def silu(values):
    return values * jax.nn.sigmoid(values)


def mixer_kernel(
    lane_ref,
    rate_ref,
    tokens_hbm,
    gain_hbm,
    decay_hbm,
    strength_hbm,
    head_gain_hbm,
    query_hbm,
    key_hbm,
    value_hbm,
    state_hbm,
    out_hbm,
    send_ref,
    keep_ref,
    retain_ref,
    corrected_ref,
    keys_ref,
    tokens_s,
    gain_s,
    gates_s,
    head_gain_s,
    proj_s,
    state_s,
    out_s,
    recall_s,
    read_s,
    sems,
):
    rows, width = tokens_s.shape
    head = head_gain_s.shape[-1]
    heads = decay_hbm.shape[0]
    chunks = 4
    step = width // chunks
    copies = []
    for c in range(chunks):
        for n, source in enumerate((query_hbm, key_hbm, value_hbm)):
            copies.append(
                pltpu.make_async_copy(
                    source.at[pl.ds(c * step, step), :],
                    proj_s.at[pl.ds(c * step, step), pl.ds(n * head, head)],
                    sems.at[c * 3 + n],
                )
            )
    base = 3 * chunks
    state_copy = pltpu.make_async_copy(state_hbm, state_s, sems.at[base])
    out_copy = pltpu.make_async_copy(out_hbm, out_s, sems.at[base + 1])
    tokens_copy = pltpu.make_async_copy(tokens_hbm, tokens_s, sems.at[base + 2])
    gain_copy = pltpu.make_async_copy(gain_hbm, gain_s, sems.at[base + 3])
    decay_copy = pltpu.make_async_copy(decay_hbm, gates_s.at[pl.ds(0, heads), :], sems.at[base + 4])
    strength_copy = pltpu.make_async_copy(
        strength_hbm, gates_s.at[pl.ds(heads, heads), :], sems.at[base + 5]
    )
    head_gain_copy = pltpu.make_async_copy(head_gain_hbm, head_gain_s, sems.at[base + 6])
    small = (gain_copy, decay_copy, strength_copy, head_gain_copy)
    tokens_copy.start()
    for copy in small:
        copy.start()
    for copy in copies:
        copy.start()
    state_copy.start()
    out_copy.start()

    tokens_copy.wait()
    values = tokens_s[...].astype(f32)
    scale = lax.rsqrt(jnp.mean(values * values, axis=-1, keepdims=True) + epsilon)
    for copy in small:
        copy.wait()
    gain = gain_s[...].astype(f32)
    normed = jnp.concatenate(
        [
            (values[:, i * head : (i + 1) * head] * scale * gain[i : i + 1, :]).astype(bf16)
            for i in range(width // head)
        ],
        axis=1,
    )

    lane = lane_ref[0]
    gates = lax.dot_general(
        normed, gates_s[...], (((1,), (1,)), ((), ())), preferred_element_type=f32
    )
    column = lax.broadcasted_iota(jnp.int32, gates.shape, 1)

    def own(place):
        return jnp.sum(jnp.where(column == place, gates, 0.0), axis=1, keepdims=True)

    decay_pre = own(lane)
    strength = jax.nn.sigmoid(own(lane + heads))
    softplus = jnp.maximum(decay_pre, 0.0) + jnp.log1p(jnp.exp(-jnp.abs(decay_pre)))
    retain = jnp.exp(-rate_ref[0] * softplus)

    total = jnp.zeros((rows, 3 * head), f32)
    for c in range(chunks):
        for copy in copies[3 * c : 3 * c + 3]:
            copy.wait()
        total = total + jnp.dot(
            normed[:, c * step : (c + 1) * step],
            proj_s[pl.ds(c * step, step), :],
            preferred_element_type=f32,
        )
    projected = total.astype(bf16).astype(f32)
    query = silu(projected[:, :head])
    key = silu(projected[:, head : 2 * head])
    value = silu(projected[:, 2 * head :])
    query = query * lax.rsqrt(jnp.sum(query * query, axis=-1, keepdims=True) + epsilon)
    query = query * head ** (-0.5)
    key = key * lax.rsqrt(jnp.sum(key * key, axis=-1, keepdims=True) + epsilon)
    match = jnp.sum(query * key, axis=-1, keepdims=True)

    fill = jnp.zeros((head - rows, head), f32)
    query_t = jnp.transpose(jnp.concatenate([query, fill], axis=0))
    key_t = jnp.transpose(jnp.concatenate([key, fill], axis=0))
    keys_ref[...] = key_t
    state_copy.wait()
    for t in range(rows):
        block = state_s[t]
        recall_s[pl.ds(t, 1), :] = jnp.sum(block * key_t[:, t : t + 1], axis=0, keepdims=True)
        read_s[pl.ds(t, 1), :] = jnp.sum(block * query_t[:, t : t + 1], axis=0, keepdims=True)
    corrected = strength * (value - retain * recall_s[...])
    readout = retain * read_s[...] + match * corrected
    retain_ref[...] = jnp.broadcast_to(retain, (rows, head))
    corrected_ref[...] = corrected
    scaled = readout * lax.rsqrt(jnp.mean(readout * readout, axis=-1, keepdims=True) + epsilon)
    mixed = (scaled * head_gain_s[...].astype(f32)).astype(bf16)

    out_copy.wait()
    share = send_ref.shape[-1]
    for k in range(4):
        near = (lane ^ (2 * k)) * share
        far = (lane ^ (2 * k + 1)) * share
        send_ref[k] = jnp.dot(
            mixed, out_s[:, pl.ds(pl.multiple_of(far, 128), share)], preferred_element_type=f32
        ).astype(bf16)
        keep_ref[k] = jnp.dot(
            mixed, out_s[:, pl.ds(pl.multiple_of(near, 128), share)], preferred_element_type=f32
        ).astype(bf16)


def state_kernel(
    after_ref, retain_ref, corrected_ref, keys_ref, state_hbm, new_hbm, done_ref, old_s, new_s, sems
):
    done_ref[...] = jnp.zeros_like(done_ref)
    rows = old_s.shape[0]
    parts = 4
    step = rows // parts

    def window(i):
        return pl.ds(i * step, step)

    loads = [
        pltpu.make_async_copy(state_hbm.at[window(i)], old_s.at[window(i)], sems.at[i])
        for i in range(parts)
    ]
    stores = [
        pltpu.make_async_copy(new_s.at[window(i)], new_hbm.at[window(i)], sems.at[parts + i])
        for i in range(parts)
    ]
    for load in loads:
        load.start()
    for i in range(parts):
        loads[i].wait()
        for t in range(i * step, (i + 1) * step):
            new_s[t] = (
                old_s[t] * retain_ref[pl.ds(t, 1), :]
                + keys_ref[:, t : t + 1] * corrected_ref[pl.ds(t, 1), :]
            )
        stores[i].start()
    for store in stores:
        store.wait()


def pair_sum_kernel(keep_ref, recv_ref, *out_refs):
    for k, out in enumerate(out_refs):
        out[...] = (keep_ref[k].astype(f32) + recv_ref[k].astype(f32)).astype(bf16)


def load_kernel(after_ref, source_hbm, target_ref, done_ref, sem):
    done_ref[...] = jnp.zeros_like(done_ref)
    copy = pltpu.make_async_copy(source_hbm, target_ref, sem)
    copy.start()
    copy.wait()


def route_kernel(capacity, after_ref, routing_ref, weight_ref, place_ref, pick_ref, spread_ref):
    top, rows = routing_ref.shape
    slots = place_ref.shape[0]
    row_id = lax.broadcasted_iota(jnp.int32, (rows, rows), 0)
    lane_id = lax.broadcasted_iota(jnp.int32, (rows, rows), 1)

    def column(line, zero):
        return jnp.sum(jnp.where(row_id == lane_id, line, zero), axis=1, keepdims=True)

    lines = [routing_ref[j : j + 1, :] for j in range(top)]
    slot_id = lax.broadcasted_iota(jnp.int32, (rows, slots), 1)
    placed = jnp.zeros((rows, slots), f32)
    for j in range(top):
        chosen = column(lines[j], 0)
        rank = jnp.zeros((rows, 1), jnp.int32)
        for line in lines:
            earlier = (chosen == line) & (lane_id < row_id)
            rank = rank + jnp.sum(earlier.astype(jnp.int32), axis=1, keepdims=True)
        pick = (slot_id == chosen * capacity + rank).astype(f32)
        placed = placed + pick
        pick_ref[j] = pick.astype(bf16)
        spread_ref[j] = jnp.broadcast_to(column(weight_ref[j : j + 1, :], 0.0), spread_ref.shape[1:])
    fill = jnp.zeros((slots - rows, slots), f32)
    place_ref[...] = jnp.transpose(jnp.concatenate([placed, fill], axis=0))[:, :rows].astype(bf16)


def join_kernel(a_ref, b_ref, c_ref, d_ref, out_ref):
    for k, part in enumerate((a_ref, b_ref, c_ref, d_ref)):
        out_ref[k] = part[...]


def residual_kernel(
    after_ref, lane_ref, tokens_ref, place_ref, a_ref, b_ref, c_ref, d_ref, own_ref, out_ref
):
    share = own_ref.shape[-1]
    start = pl.multiple_of(lane_ref[0] * share, 128)
    mix = (a_ref[...].astype(f32) + b_ref[...].astype(f32)) + (
        c_ref[...].astype(f32) + d_ref[...].astype(f32)
    )
    own = (tokens_ref[:, pl.ds(start, share)].astype(f32) + mix).astype(bf16)
    own_ref[...] = own
    out_ref[...] = jnp.dot(place_ref[...], own, preferred_element_type=f32).astype(bf16)


def expert_kernel(
    lane_ref,
    gain_ref,
    near_ref,
    far_ref,
    gate_ref,
    up_hbm,
    down_hbm,
    send_ref,
    keep_ref,
    up_ref,
    down_ref,
    fed_ref,
    sems,
):
    up_copy = pltpu.make_async_copy(up_hbm, up_ref, sems.at[0])
    down_copy = pltpu.make_async_copy(down_hbm, down_ref, sems.at[1])
    up_copy.start()
    down_copy.start()
    rows, share = near_ref.shape[1:]
    head = gain_ref.shape[-1]
    lane = lane_ref[0]
    starts = [pl.multiple_of((lane ^ k) * share, 128) for k in range(8)]
    pieces = [(far_ref if k % 2 else near_ref).at[k // 2] for k in range(8)]
    square = jnp.zeros((rows, 1), f32)
    for k in range(8):
        values = pieces[k][...].astype(f32)
        square = square + jnp.sum(values * values, axis=-1, keepdims=True)
    scale = lax.rsqrt(square / (8 * share) + epsilon)
    gate_pre = jnp.zeros((rows, gate_ref.shape[-1]), f32)
    up_pre = jnp.zeros((rows, gate_ref.shape[-1]), f32)
    for k in range(8):
        values = pieces[k][...].astype(f32)
        gain = gain_ref[pl.ds((lane ^ k) * (share // head), share // head), :]
        fed = jnp.concatenate(
            [
                (values[:, i * head : (i + 1) * head] * scale * gain[i : i + 1, :]).astype(bf16)
                for i in range(share // head)
            ],
            axis=1,
        )
        fed_ref[k] = fed
        window = pl.ds(starts[k], share)
        gate_pre = gate_pre + jnp.dot(fed, gate_ref[window, :], preferred_element_type=f32)
    up_copy.wait()
    for k in range(8):
        window = pl.ds(starts[k], share)
        up_pre = up_pre + jnp.dot(fed_ref[k], up_ref[window, :], preferred_element_type=f32)
    gate_cut = jnp.minimum(gate_pre, clamp_limit)
    up_cut = jnp.clip(up_pre, -clamp_limit, clamp_limit)
    hidden = ((up_cut + 1.0) * gate_cut * jax.nn.sigmoid(swish_alpha * gate_cut)).astype(bf16)
    down_copy.wait()
    for k in range(4):
        send_ref[k] = jnp.dot(
            hidden, down_ref[:, pl.ds(starts[2 * k + 1], share)], preferred_element_type=f32
        ).astype(bf16)
        keep_ref[k] = jnp.dot(
            hidden, down_ref[:, pl.ds(starts[2 * k], share)], preferred_element_type=f32
        ).astype(bf16)


def total_kernel(after_ref, a_ref, b_ref, c_ref, d_ref, out_ref):
    out_ref[...] = (
        (a_ref[...].astype(f32) + b_ref[...].astype(f32))
        + (c_ref[...].astype(f32) + d_ref[...].astype(f32))
    ).astype(bf16)


def combine_kernel(own_ref, picks_ref, spread_ref, back_ref, out_ref):
    back = back_ref[...]
    total = own_ref[...].astype(f32)
    for j in range(picks_ref.shape[0]):
        picked = jnp.dot(picks_ref[j], back, preferred_element_type=f32)
        total = total + picked * spread_ref[j][:, :1]
    out_ref[...] = total.astype(bf16)


def on_device(
    tokens,
    mix_gain,
    query_weight,
    key_weight,
    value_weight,
    decay_weight,
    strength_weight,
    decay_rate,
    head_gain,
    memory_state,
    output_weight,
    ffn_gain,
    routing,
    route_weight,
    expert_gate,
    expert_up,
    expert_down,
):
    groups = lax.axis_size("ep")
    lane = lax.axis_index("tp").astype(jnp.int32).reshape(1)
    rows, width = tokens.shape
    head = memory_state.shape[-1]
    share = width // 8
    hidden_units = expert_gate.shape[-1]
    top = routing.shape[1]
    capacity = 2 * rows * top // groups
    slots = groups * capacity
    limits = pltpu.CompilerParams(vmem_limit_bytes=24 * 2**20)

    def across(array, flip):
        return lax.ppermute(array, "tp", [(i, i ^ flip) for i in range(8)])

    state = memory_state.reshape(rows, head, head)
    send, keep, retain, corrected, keys = pl.pallas_call(
        mixer_kernel,
        out_shape=(
            shaped((4, rows, share), bf16),
            shaped((4, rows, share), bf16),
            shaped((rows, head), f32),
            shaped((rows, head), f32),
            shaped((head, head), f32),
        ),
        in_specs=[in_smem()] * 2 + [in_hbm()] * 10,
        out_specs=(in_vmem(),) * 5,
        scratch_shapes=[
            VMEM((rows, width), bf16),
            VMEM((width // head, head), bf16),
            VMEM((2 * decay_weight.shape[1], width), bf16),
            VMEM((1, head), bf16),
            VMEM((width, 3 * head), bf16),
            VMEM((rows, head, head), f32),
            VMEM((head, width), bf16),
            VMEM((rows, head), f32),
            VMEM((rows, head), f32),
            pltpu.SemaphoreType.DMA((20,)),
        ],
        compiler_params=limits,
        name="mixer",
    )(
        lane,
        decay_rate,
        *[
            pinned(array)
            for array in (
                tokens,
                mix_gain.reshape(width // head, head),
                decay_weight.T,
                strength_weight.T,
                head_gain.reshape(1, head),
                query_weight,
                key_weight,
                value_weight,
                state,
                output_weight,
            )
        ],
    )
    recv = across(send, 1)
    place, picks, spread = pl.pallas_call(
        partial(route_kernel, capacity),
        out_shape=(
            shaped((slots, rows), bf16),
            shaped((top, rows, slots), bf16),
            shaped((top, rows, 128), f32),
        ),
        in_specs=[in_any()] + [in_vmem()] * 2,
        out_specs=(in_vmem(),) * 3,
        compiler_params=limits,
        name="route",
    )(retain, routing.T, route_weight.T)

    def pair_sums(keep, recv):
        shape = keep.shape[1:]
        return pl.pallas_call(
            pair_sum_kernel,
            out_shape=(shaped(shape, bf16),) * 4,
            in_specs=[in_vmem()] * 2,
            out_specs=(in_vmem(),) * 4,
            compiler_params=limits,
            name="pair_sum",
        )(keep, recv)

    sums = pair_sums(keep, recv)
    gathered = [sums[0]] + [across(sums[k], 2 * k) for k in (1, 2, 3)]

    gate, loaded = pl.pallas_call(
        load_kernel,
        out_shape=(VMEM((width, hidden_units), bf16), VMEM((8, 128), f32)),
        in_specs=[in_any(), in_hbm()],
        out_specs=(in_vmem(),) * 2,
        scratch_shapes=[pltpu.SemaphoreType.DMA],
        compiler_params=limits,
        name="load",
    )(sums[0], pinned(expert_gate.reshape(width, hidden_units)))

    own, outgoing = pl.pallas_call(
        residual_kernel,
        out_shape=(shaped((rows, share), bf16), shaped((slots, share), bf16)),
        in_specs=[in_any(), in_smem()] + [in_vmem()] * 6,
        out_specs=(in_vmem(),) * 2,
        compiler_params=limits,
        name="residual",
    )(loaded, lane, tokens, place, *gathered)

    def exchanged(array):
        blocks = array.reshape(groups, capacity, share)
        return lax.all_to_all(blocks, "ep", 0, 0, tiled=True).reshape(slots, share)

    arrived = exchanged(outgoing)
    near = [arrived] + [across(arrived, 2 * k) for k in (1, 2, 3)]
    near = pl.pallas_call(
        join_kernel,
        out_shape=shaped((4, slots, share), bf16),
        in_specs=[in_vmem()] * 4,
        out_specs=in_vmem(),
        compiler_params=limits,
        name="join",
    )(*near)
    far = across(near, 1)

    send, keep = pl.pallas_call(
        expert_kernel,
        out_shape=(shaped((4, slots, share), bf16),) * 2,
        in_specs=[in_smem()] + [in_vmem()] * 4 + [in_hbm()] * 2,
        out_specs=(in_vmem(),) * 2,
        scratch_shapes=[
            VMEM((width, hidden_units), bf16),
            VMEM((hidden_units, width), bf16),
            VMEM((8, slots, share), bf16),
            pltpu.SemaphoreType.DMA((2,)),
        ],
        compiler_params=limits,
        name="expert",
    )(
        lane,
        ffn_gain.reshape(width // head, head).astype(f32),
        near,
        far,
        gate,
        pinned(expert_up.reshape(width, hidden_units)),
        pinned(expert_down.reshape(hidden_units, width)),
    )
    recv = across(send, 1)
    sums = pair_sums(keep, recv)
    gathered = [sums[0]] + [across(sums[k], 2 * k) for k in (1, 2, 3)]
    new_state, stored = pl.pallas_call(
        state_kernel,
        out_shape=(shaped(state.shape, f32), VMEM((8, 128), f32)),
        in_specs=[in_any()] + [in_vmem()] * 3 + [in_hbm()],
        out_specs=(in_hbm(), in_vmem()),
        scratch_shapes=[
            VMEM(state.shape, f32),
            VMEM(state.shape, f32),
            pltpu.SemaphoreType.DMA((8,)),
        ],
        compiler_params=limits,
        name="state",
    )(sums[0], retain, corrected, keys, pinned(state))

    expert_out = pl.pallas_call(
        total_kernel,
        out_shape=shaped((slots, share), bf16),
        in_specs=[in_any()] + [in_vmem()] * 4,
        out_specs=in_vmem(),
        compiler_params=limits,
        name="total",
    )(stored, *gathered)
    back = exchanged(expert_out)
    layer_out = pl.pallas_call(
        combine_kernel,
        out_shape=shaped((rows, share), bf16),
        in_specs=[in_vmem()] * 4,
        out_specs=in_vmem(),
        compiler_params=limits,
        name="combine",
    )(own, picks, spread, back)
    return layer_out, new_state.reshape(memory_state.shape)


def solution(mesh):
    placed = (
        P("ep", None),
        P(),
        P(None, "tp"),
        P(None, "tp"),
        P(None, "tp"),
        P(),
        P(),
        P("tp"),
        P(),
        P("ep", "tp", None, None),
        P("tp", None),
        P(),
        P("ep", None),
        P("ep", None),
        P("ep", None, "tp"),
        P("ep", None, "tp"),
        P("ep", "tp", None),
    )
    return jax.shard_map(
        on_device,
        mesh=mesh,
        in_specs=placed,
        out_specs=(P("ep", "tp"), P("ep", "tp", None, None)),
        check_vma=False,
    )
```

```python
from functools import partial

import jax
import jax.numpy as jnp
from jax import lax
from jax.experimental import pallas as pl
from jax.experimental.pallas import tpu as pltpu
from jax.sharding import PartitionSpec as P

epsilon = 1e-06
clamp_limit = 7.0
swish_alpha = 1.702
f32 = jnp.float32
bf16 = jnp.bfloat16


VMEM = pltpu.VMEM
SMEM = pltpu.SMEM


def in_vmem():
    return pl.BlockSpec(memory_space=VMEM)


def in_smem():
    return pl.BlockSpec(memory_space=SMEM)


def in_hbm():
    return pl.BlockSpec(memory_space=pltpu.HBM)


def in_any():
    return pl.BlockSpec(memory_space=pl.ANY)


def pinned(array):
    return pltpu.with_memory_space_constraint(array, pltpu.HBM)


def shaped(shape, dtype):
    return jax.ShapeDtypeStruct(shape, dtype)


def silu(values):
    return values * jax.nn.sigmoid(values)


def mixer_kernel(
    lane_ref,
    rate_ref,
    tokens_hbm,
    gain_hbm,
    decay_hbm,
    strength_hbm,
    head_gain_hbm,
    query_hbm,
    key_hbm,
    value_hbm,
    state_hbm,
    out_hbm,
    send_ref,
    keep_ref,
    retain_ref,
    corrected_ref,
    keys_ref,
    tokens_s,
    gain_s,
    gates_s,
    head_gain_s,
    proj_s,
    state_s,
    out_s,
    recall_s,
    read_s,
    sems,
):
    rows, width = tokens_s.shape
    head = head_gain_s.shape[-1]
    heads = decay_hbm.shape[0]
    chunks = 4
    step = width // chunks
    copies = []
    for c in range(chunks):
        for n, source in enumerate((query_hbm, key_hbm, value_hbm)):
            copies.append(
                pltpu.make_async_copy(
                    source.at[pl.ds(c * step, step), :],
                    proj_s.at[pl.ds(c * step, step), pl.ds(n * head, head)],
                    sems.at[c * 3 + n],
                )
            )
    base = 3 * chunks
    state_copy = pltpu.make_async_copy(state_hbm, state_s, sems.at[base])
    lane = lane_ref[0]
    out_copy = pltpu.make_async_copy(out_hbm, out_s, sems.at[base + 1])
    tokens_copy = pltpu.make_async_copy(tokens_hbm, tokens_s, sems.at[base + 2])
    gain_copy = pltpu.make_async_copy(gain_hbm, gain_s, sems.at[base + 3])
    decay_copy = pltpu.make_async_copy(decay_hbm, gates_s.at[pl.ds(0, heads), :], sems.at[base + 4])
    strength_copy = pltpu.make_async_copy(
        strength_hbm, gates_s.at[pl.ds(heads, heads), :], sems.at[base + 5]
    )
    head_gain_copy = pltpu.make_async_copy(head_gain_hbm, head_gain_s, sems.at[base + 6])
    small = (gain_copy, decay_copy, strength_copy, head_gain_copy)
    tokens_copy.start()
    for copy in small:
        copy.start()
    for copy in copies:
        copy.start()
    state_copy.start()
    out_copy.start()

    tokens_copy.wait()
    values = tokens_s[...].astype(f32)
    scale = lax.rsqrt(jnp.mean(values * values, axis=-1, keepdims=True) + epsilon)
    for copy in small:
        copy.wait()
    gain = gain_s[...].astype(f32)
    normed = jnp.concatenate(
        [
            (values[:, i * head : (i + 1) * head] * scale * gain[i : i + 1, :]).astype(bf16)
            for i in range(width // head)
        ],
        axis=1,
    )

    gates = lax.dot_general(
        normed, gates_s[...], (((1,), (1,)), ((), ())), preferred_element_type=f32
    )
    column = lax.broadcasted_iota(jnp.int32, gates.shape, 1)

    def own(place):
        return jnp.sum(jnp.where(column == place, gates, 0.0), axis=1, keepdims=True)

    decay_pre = own(lane)
    strength = jax.nn.sigmoid(own(lane + heads))
    softplus = jnp.maximum(decay_pre, 0.0) + jnp.log1p(jnp.exp(-jnp.abs(decay_pre)))
    retain = jnp.exp(-rate_ref[0] * softplus)

    total = jnp.zeros((rows, 3 * head), f32)
    for c in range(chunks):
        for copy in copies[3 * c : 3 * c + 3]:
            copy.wait()
        total = total + jnp.dot(
            normed[:, c * step : (c + 1) * step],
            proj_s[pl.ds(c * step, step), :],
            preferred_element_type=f32,
        )
    projected = total.astype(bf16).astype(f32)
    query = silu(projected[:, :head])
    key = silu(projected[:, head : 2 * head])
    value = silu(projected[:, 2 * head :])
    query = query * lax.rsqrt(jnp.sum(query * query, axis=-1, keepdims=True) + epsilon)
    query = query * head ** (-0.5)
    key = key * lax.rsqrt(jnp.sum(key * key, axis=-1, keepdims=True) + epsilon)
    match = jnp.sum(query * key, axis=-1, keepdims=True)

    fill = jnp.zeros((head - rows, head), f32)
    query_t = jnp.transpose(jnp.concatenate([query, fill], axis=0))
    key_t = jnp.transpose(jnp.concatenate([key, fill], axis=0))
    keys_ref[...] = key_t
    state_copy.wait()
    for t in range(rows):
        block = state_s[t]
        recall_s[pl.ds(t, 1), :] = jnp.sum(block * key_t[:, t : t + 1], axis=0, keepdims=True)
        read_s[pl.ds(t, 1), :] = jnp.sum(block * query_t[:, t : t + 1], axis=0, keepdims=True)
    corrected = strength * (value - retain * recall_s[...])
    readout = retain * read_s[...] + match * corrected
    retain_ref[...] = jnp.broadcast_to(retain, (rows, head))
    corrected_ref[...] = corrected
    scaled = readout * lax.rsqrt(jnp.mean(readout * readout, axis=-1, keepdims=True) + epsilon)
    mixed = (scaled * head_gain_s[...].astype(f32)).astype(bf16)

    out_copy.wait()
    share = send_ref.shape[-1]
    for k in range(4):
        far = pl.multiple_of((lane ^ (2 * k + 1)) * share, 128)
        send_ref[k] = jnp.dot(
            mixed, out_s[:, pl.ds(far, share)], preferred_element_type=f32
        ).astype(bf16)
    for k in range(4):
        near = pl.multiple_of((lane ^ (2 * k)) * share, 128)
        keep_ref[k] = jnp.dot(
            mixed, out_s[:, pl.ds(near, share)], preferred_element_type=f32
        ).astype(bf16)


def state_kernel(
    after_ref, retain_ref, corrected_ref, keys_ref, state_hbm, new_hbm, done_ref, old_s, new_s, sems
):
    done_ref[...] = jnp.zeros_like(done_ref)
    rows = old_s.shape[0]
    parts = 4
    step = rows // parts

    def window(i):
        return pl.ds(i * step, step)

    loads = [
        pltpu.make_async_copy(state_hbm.at[window(i)], old_s.at[window(i)], sems.at[i])
        for i in range(parts)
    ]
    stores = [
        pltpu.make_async_copy(new_s.at[window(i)], new_hbm.at[window(i)], sems.at[parts + i])
        for i in range(parts)
    ]
    for load in loads:
        load.start()
    for i in range(parts):
        loads[i].wait()
        for t in range(i * step, (i + 1) * step):
            new_s[t] = (
                old_s[t] * retain_ref[pl.ds(t, 1), :]
                + keys_ref[:, t : t + 1] * corrected_ref[pl.ds(t, 1), :]
            )
        stores[i].start()
    for store in stores:
        store.wait()


def pair_sum_kernel(keep_ref, recv_ref, *out_refs):
    for k, out in enumerate(out_refs):
        out[...] = (keep_ref[k].astype(f32) + recv_ref[k].astype(f32)).astype(bf16)


def load_kernel(after_ref, *refs):
    count = len(refs) // 2 - 1
    done_ref, sems = refs[-2:]
    done_ref[...] = jnp.zeros_like(done_ref)
    copies = [
        pltpu.make_async_copy(refs[i], refs[count + i], sems.at[i]) for i in range(count)
    ]
    for copy in copies:
        copy.start()
    for copy in copies:
        copy.wait()


def route_kernel(capacity, after_ref, routing_ref, weight_ref, place_ref, pick_ref, spread_ref):
    top, rows = routing_ref.shape
    slots = place_ref.shape[0]
    row_id = lax.broadcasted_iota(jnp.int32, (rows, rows), 0)
    lane_id = lax.broadcasted_iota(jnp.int32, (rows, rows), 1)

    def column(line, zero):
        return jnp.sum(jnp.where(row_id == lane_id, line, zero), axis=1, keepdims=True)

    lines = [routing_ref[j : j + 1, :] for j in range(top)]
    slot_id = lax.broadcasted_iota(jnp.int32, (rows, slots), 1)
    placed = jnp.zeros((rows, slots), f32)
    for j in range(top):
        chosen = column(lines[j], 0)
        rank = jnp.zeros((rows, 1), jnp.int32)
        for line in lines:
            earlier = (chosen == line) & (lane_id < row_id)
            rank = rank + jnp.sum(earlier.astype(jnp.int32), axis=1, keepdims=True)
        pick = (slot_id == chosen * capacity + rank).astype(f32)
        placed = placed + pick
        pick_ref[j] = pick.astype(bf16)
        spread_ref[j] = jnp.broadcast_to(column(weight_ref[j : j + 1, :], 0.0), spread_ref.shape[1:])
    fill = jnp.zeros((slots - rows, slots), f32)
    place_ref[...] = jnp.transpose(jnp.concatenate([placed, fill], axis=0))[:, :rows].astype(bf16)


def join_kernel(after_ref, a_ref, b_ref, c_ref, d_ref, out_ref):
    for k, part in enumerate((a_ref, b_ref, c_ref, d_ref)):
        out_ref[k] = part[...].reshape(out_ref.shape[1:])


def residual_kernel(
    after_ref, lane_ref, tokens_ref, place_ref, a_ref, b_ref, c_ref, d_ref, own_ref, out_ref
):
    share = own_ref.shape[-1]
    start = pl.multiple_of(lane_ref[0] * share, 128)
    mix = (a_ref[...].astype(f32) + b_ref[...].astype(f32)) + (
        c_ref[...].astype(f32) + d_ref[...].astype(f32)
    )
    own = (tokens_ref[:, pl.ds(start, share)].astype(f32) + mix).astype(bf16)
    own_ref[...] = own
    placed = jnp.dot(place_ref[...], own, preferred_element_type=f32).astype(bf16)
    out_ref[...] = placed.reshape(out_ref.shape)


def fed_rows(values, gain_ref, lane, flip):
    head = gain_ref.shape[-1]
    blocks = values.shape[-1] // head
    gain = gain_ref[pl.ds((lane ^ flip) * blocks, blocks), :]
    return jnp.concatenate(
        [
            (values[:, i * head : (i + 1) * head] * gain[i : i + 1, :]).astype(bf16)
            for i in range(blocks)
        ],
        axis=1,
    )


def near_kernel(
    lane_ref, gain_ref, near_ref, gate_ref, up_ref, gate_out, up_out, square_out
):
    rows, share = near_ref.shape[1:]
    lane = lane_ref[0]
    square = jnp.zeros((rows, 1), f32)
    gate_pre = jnp.zeros(gate_out.shape, f32)
    up_pre = jnp.zeros(up_out.shape, f32)
    for k in range(4):
        values = near_ref[k].astype(f32)
        square = square + jnp.sum(values * values, axis=-1, keepdims=True)
        fed = fed_rows(values, gain_ref, lane, 2 * k)
        window = pl.ds(pl.multiple_of((lane ^ (2 * k)) * share, 128), share)
        gate_pre = gate_pre + jnp.dot(fed, gate_ref[window, :], preferred_element_type=f32)
        up_pre = up_pre + jnp.dot(fed, up_ref[window, :], preferred_element_type=f32)
    gate_out[...] = gate_pre
    up_out[...] = up_pre
    square_out[...] = jnp.broadcast_to(square, square_out.shape)


def far_kernel(
    lane_ref,
    gain_ref,
    far_ref,
    gate_ref,
    up_ref,
    gate_near,
    up_near,
    square_near,
    down_ref,
    send_ref,
    hidden_ref,
):
    share = far_ref.shape[-1]
    lane = lane_ref[0]
    square = square_near[:, 0:1]
    gate_pre = gate_near[...]
    up_pre = up_near[...]
    for k in range(4):
        values = far_ref[k].astype(f32)
        square = square + jnp.sum(values * values, axis=-1, keepdims=True)
        fed = fed_rows(values, gain_ref, lane, 2 * k + 1)
        window = pl.ds(pl.multiple_of((lane ^ (2 * k + 1)) * share, 128), share)
        gate_pre = gate_pre + jnp.dot(fed, gate_ref[window, :], preferred_element_type=f32)
        up_pre = up_pre + jnp.dot(fed, up_ref[window, :], preferred_element_type=f32)
    scale = lax.rsqrt(square / (8 * share) + epsilon)
    gate_cut = jnp.minimum(gate_pre * scale, clamp_limit)
    up_cut = jnp.clip(up_pre * scale, -clamp_limit, clamp_limit)
    hidden = ((up_cut + 1.0) * gate_cut * jax.nn.sigmoid(swish_alpha * gate_cut)).astype(bf16)
    hidden_ref[...] = hidden
    for k in range(4):
        window = pl.ds(pl.multiple_of((lane ^ (2 * k + 1)) * share, 128), share)
        send_ref[k] = jnp.dot(
            hidden, down_ref[:, window], preferred_element_type=f32
        ).astype(bf16)


def kept_kernel(lane_ref, hidden_ref, down_ref, keep_ref):
    share = keep_ref.shape[-1]
    hidden = hidden_ref[...]
    for k in range(4):
        window = pl.ds(pl.multiple_of((lane_ref[0] ^ (2 * k)) * share, 128), share)
        keep_ref[k] = jnp.dot(
            hidden, down_ref[:, window], preferred_element_type=f32
        ).astype(bf16)


def total_kernel(after_ref, a_ref, b_ref, c_ref, d_ref, out_ref):
    total = (
        (a_ref[...].astype(f32) + b_ref[...].astype(f32))
        + (c_ref[...].astype(f32) + d_ref[...].astype(f32))
    ).astype(bf16)
    out_ref[...] = total.reshape(out_ref.shape)


def combine_kernel(own_ref, picks_ref, spread_ref, back_ref, out_ref):
    groups, capacity, share = back_ref.shape
    back = back_ref[...].reshape(groups * capacity, share)
    total = own_ref[...].astype(f32)
    for j in range(picks_ref.shape[0]):
        picked = jnp.dot(picks_ref[j], back, preferred_element_type=f32)
        total = total + picked * spread_ref[j][:, :1]
    out_ref[...] = total.astype(bf16)


def on_device(
    tokens,
    mix_gain,
    query_weight,
    key_weight,
    value_weight,
    decay_weight,
    strength_weight,
    decay_rate,
    head_gain,
    memory_state,
    output_weight,
    ffn_gain,
    routing,
    route_weight,
    expert_gate,
    expert_up,
    expert_down,
):
    groups = lax.axis_size("ep")
    lane = lax.axis_index("tp").astype(jnp.int32).reshape(1)
    rows, width = tokens.shape
    head = memory_state.shape[-1]
    share = width // 8
    hidden_units = expert_gate.shape[-1]
    top = routing.shape[1]
    capacity = 2 * rows * top // groups
    slots = groups * capacity
    limits = pltpu.CompilerParams(vmem_limit_bytes=20 * 2**20)

    def across(array, flip):
        return lax.ppermute(array, "tp", [(i, i ^ flip) for i in range(8)])

    state = memory_state.reshape(rows, head, head)
    send, keep, retain, corrected, keys = pl.pallas_call(
        mixer_kernel,
        out_shape=(
            shaped((4, rows, share), bf16),
            shaped((4, rows, share), bf16),
            shaped((rows, head), f32),
            shaped((rows, head), f32),
            shaped((head, head), f32),
        ),
        in_specs=[in_smem()] * 2 + [in_hbm()] * 10,
        out_specs=(in_vmem(),) * 5,
        scratch_shapes=[
            VMEM((rows, width), bf16),
            VMEM((width // head, head), bf16),
            VMEM((2 * decay_weight.shape[1], width), bf16),
            VMEM((1, head), bf16),
            VMEM((width, 3 * head), bf16),
            VMEM((rows, head, head), f32),
            VMEM((head, width), bf16),
            VMEM((rows, head), f32),
            VMEM((rows, head), f32),
            pltpu.SemaphoreType.DMA((20,)),
        ],
        compiler_params=limits,
        name="mixer",
    )(
        lane,
        decay_rate,
        *[
            pinned(array)
            for array in (
                tokens,
                mix_gain.reshape(width // head, head),
                decay_weight.T,
                strength_weight.T,
                head_gain.reshape(1, head),
                query_weight,
                key_weight,
                value_weight,
                state,
                output_weight,
            )
        ],
    )
    recv = across(send, 1)

    place, picks, spread = pl.pallas_call(
        partial(route_kernel, capacity),
        out_shape=(
            shaped((slots, rows), bf16),
            shaped((top, rows, slots), bf16),
            shaped((top, rows, 128), f32),
        ),
        in_specs=[in_any()] + [in_vmem()] * 2,
        out_specs=(in_vmem(),) * 3,
        compiler_params=limits,
        name="route",
    )(retain, routing.T, route_weight.T)

    def pair_sums(keep, recv):
        shape = keep.shape[1:]
        return pl.pallas_call(
            pair_sum_kernel,
            out_shape=(shaped(shape, bf16),) * 4,
            in_specs=[in_vmem()] * 2,
            out_specs=(in_vmem(),) * 4,
            compiler_params=limits,
            name="pair_sum",
        )(keep, recv)

    sums = pair_sums(keep, recv)
    gathered = [sums[0]] + [across(sums[k], 2 * k) for k in (1, 2, 3)]

    def loaded(after, *arrays):
        count = len(arrays)
        return pl.pallas_call(
            load_kernel,
            out_shape=tuple(VMEM(array.shape, array.dtype) for array in arrays)
            + (VMEM((8, 128), f32),),
            in_specs=[in_any()] + [in_hbm()] * count,
            out_specs=(in_vmem(),) * (count + 1),
            scratch_shapes=[pltpu.SemaphoreType.DMA((count,))],
            compiler_params=limits,
            name="load",
        )(after, *[pinned(array) for array in arrays])

    gate, up, ready = loaded(
        sums[0],
        expert_gate.reshape(width, hidden_units),
        expert_up.reshape(width, hidden_units),
    )
    gain = ffn_gain.reshape(width // head, head).astype(f32)

    own, outgoing = pl.pallas_call(
        residual_kernel,
        out_shape=(shaped((rows, share), bf16), shaped((groups, capacity, share), bf16)),
        in_specs=[in_any(), in_smem()] + [in_vmem()] * 6,
        out_specs=(in_vmem(),) * 2,
        compiler_params=limits,
        name="residual",
    )(ready, lane, tokens, place, *gathered)

    arrived = lax.all_to_all(outgoing, "ep", 0, 0, tiled=True)
    near = [arrived] + [across(arrived, 2 * k) for k in (1, 2, 3)]
    down, ready = loaded(arrived, expert_down.reshape(hidden_units, width))
    near = pl.pallas_call(
        join_kernel,
        out_shape=shaped((4, slots, share), bf16),
        in_specs=[in_any()] + [in_vmem()] * 4,
        out_specs=in_vmem(),
        compiler_params=limits,
        name="join",
    )(ready, *near)
    far = across(near, 1)

    gate_near, up_near, square_near = pl.pallas_call(
        near_kernel,
        out_shape=(
            shaped((slots, hidden_units), f32),
            shaped((slots, hidden_units), f32),
            shaped((slots, head), f32),
        ),
        in_specs=[in_smem()] + [in_vmem()] * 4,
        out_specs=(in_vmem(),) * 3,
        compiler_params=limits,
        name="near",
    )(lane, gain, near, gate, up)
    send, hidden = pl.pallas_call(
        far_kernel,
        out_shape=(shaped((4, slots, share), bf16), shaped((slots, hidden_units), bf16)),
        in_specs=[in_smem()] + [in_vmem()] * 8,
        out_specs=(in_vmem(),) * 2,
        compiler_params=limits,
        name="far",
    )(lane, gain, far, gate, up, gate_near, up_near, square_near, down)
    recv = across(send, 1)
    keep = pl.pallas_call(
        kept_kernel,
        out_shape=shaped((4, slots, share), bf16),
        in_specs=[in_smem()] + [in_vmem()] * 2,
        out_specs=in_vmem(),
        compiler_params=limits,
        name="kept",
    )(lane, hidden, down)
    sums = pair_sums(keep, recv)
    gathered = [sums[0]] + [across(sums[k], 2 * k) for k in (1, 2, 3)]
    new_state, stored = pl.pallas_call(
        state_kernel,
        out_shape=(shaped(state.shape, f32), VMEM((8, 128), f32)),
        in_specs=[in_any()] + [in_vmem()] * 3 + [in_hbm()],
        out_specs=(in_hbm(), in_vmem()),
        scratch_shapes=[
            VMEM(state.shape, f32),
            VMEM(state.shape, f32),
            pltpu.SemaphoreType.DMA((8,)),
        ],
        compiler_params=limits,
        name="state",
    )(sums[0], retain, corrected, keys, pinned(state))

    expert_out = pl.pallas_call(
        total_kernel,
        out_shape=shaped((groups, capacity, share), bf16),
        in_specs=[in_any()] + [in_vmem()] * 4,
        out_specs=in_vmem(),
        compiler_params=limits,
        name="total",
    )(stored, *gathered)
    back = lax.all_to_all(expert_out, "ep", 0, 0, tiled=True)
    layer_out = pl.pallas_call(
        combine_kernel,
        out_shape=shaped((rows, share), bf16),
        in_specs=[in_vmem()] * 4,
        out_specs=in_vmem(),
        compiler_params=limits,
        name="combine",
    )(own, picks, spread, back)
    return layer_out, new_state.reshape(memory_state.shape)


def solution(mesh):
    placed = (
        P("ep", None),
        P(),
        P(None, "tp"),
        P(None, "tp"),
        P(None, "tp"),
        P(),
        P(),
        P("tp"),
        P(),
        P("ep", "tp", None, None),
        P("tp", None),
        P(),
        P("ep", None),
        P("ep", None),
        P("ep", None, "tp"),
        P("ep", None, "tp"),
        P("ep", "tp", None),
    )
    return jax.shard_map(
        on_device,
        mesh=mesh,
        in_specs=placed,
        out_specs=(P("ep", "tp"), P("ep", "tp", None, None)),
        check_vma=False,
    )
```
